32 devices in a mesh: sp: 8 (over z, y), tp: 4 (over x, core).
Axes of the slice: x: 2, y: 2, z: 4, core: 2. Of those that a mesh axis runs over, the one named last changes fastest.
Arguments:
- tokens: bfloat16 [4096, 2048], P(('sp', 'tp')), may hold values from -6 to 6
- queries: bfloat16 [4096, 1024], P('sp', 'tp'), may hold values from -160 to 160
- keys: bfloat16 [4096, 1024], P('sp', 'tp'), may hold values from -8 to 8
- values: bfloat16 [4096, 1024], P('sp', 'tp'), may hold values from -6 to 6
- lambdas: float32 [8], P('tp'), may hold values from 0.3 to 0.8
- head_gain: float32 [128], replicated, may hold values from 0.1 to 1.9
- out_weight: bfloat16 [1024, 2048], replicated, may hold values from -0.1875 to 0.1875
- mixer_gain: float32 [2048], replicated, may hold values from 0.1 to 1.9
- up_weight: bfloat16 [2048, 4096], P('sp', 'tp'), may hold values from -0.125 to 0.125
- down_weight: bfloat16 [4096, 2048], P('tp', 'sp'), may hold values from -0.09375 to 0.09375
Outputs:
- result: bfloat16 [4096, 2048], P(('sp', 'tp'))
The draws below stay inside these ranges and needn't reach their ends.
All inputs are finite; a program needn't handle non-finite values.
Results may differ from the reference program's by a relative error of at most 0.02.
Values may be sent and summed in bfloat16 or wider, within the bound.
A program may use at most 128 MiB of HBM per device.

```python
import math
import jax
import jax.numpy as jnp
from jax import lax

D = 2048
HEADS = 8
DQK = 64
DV = 128
ATTN = 1024
FF = 4096
TOKENS = 4096


def drawn(key):
    base = jax.random.normal(jax.random.fold_in(key, 11), (TOKENS, HEADS * 2 * DQK), jnp.float32) * 1.3
    base = jnp.clip(base, -7.8, 7.8)
    return base


def draw_keys(key, part):
    base = drawn(key)
    return base.astype(jnp.bfloat16)


def draw_queries(key, part):
    own = jax.random.normal(jax.random.fold_in(key, 21), (TOKENS, HEADS * 2 * DQK), jnp.float32) * 1.3
    own = jnp.clip(own, -7.8, 7.8)
    return own.astype(jnp.bfloat16)


def steps_of(own_key, shape, pieces, least, top_value):
    loudness = 1.0
    for position, blocks in pieces:
        steps = jax.random.uniform(jax.random.fold_in(jax.random.fold_in(own_key, 6), position), (blocks,), jnp.float32, least / len(pieces), top_value / len(pieces))
        loudness = loudness * jnp.repeat(jnp.exp(steps), shape[position] // blocks).reshape((-1,) + (1,) * (len(shape) - 1 - position))
    return loudness


def bell_draw(key, dims, width, most, cuts=(), kind=jnp.bfloat16):
    entries = jax.random.normal(key, dims, jnp.float32) * width
    if len(cuts) > 0:
        entries = steps_of(key, dims, cuts, -0.22, 0.18) * entries
    return jnp.clip(entries, min=-most, max=most).astype(kind)


def setup_inputs(seed: int = 0) -> dict:
    splits = jax.random.split(jax.random.key(seed), 11)
    tokens = bell_draw(splits[0], (TOKENS, D), 1.0, 6.0, ((0, 32),))
    queries = draw_queries(jax.random.fold_in(splits[10], 71), 0)
    keys = draw_keys(jax.random.fold_in(splits[10], 71), 0)
    values = bell_draw(splits[3], (TOKENS, ATTN), 1.0, 6.0, ((0, 8), (1, 4)))
    lambdas = jnp.clip(0.3 + 0.5 * jax.random.uniform(splits[4], (HEADS,), jnp.float32) ** steps_of(splits[4], (HEADS,), ((0, 4),), -0.2, 0.2), 0.3, 0.8)
    head_gain = jnp.clip(1.0 + 0.18 * jax.random.normal(splits[5], (DV,), jnp.float32), 0.1, 1.9)
    out_weight = bell_draw(splits[6], (ATTN, D), ATTN ** -0.5, 0.1875)
    mixer_gain = jnp.clip(1.0 + 0.18 * jax.random.normal(splits[7], (D,), jnp.float32), 0.1, 1.9)
    up_weight = bell_draw(splits[8], (D, FF), D ** -0.5, 0.125, ((0, 8), (1, 4)))
    down_weight = bell_draw(splits[9], (FF, D), FF ** -0.5, 0.09375, ((0, 4), (1, 8)))
    return {"tokens": tokens, "queries": queries, "keys": keys, "values": values, "lambdas": lambdas, "head_gain": head_gain, "out_weight": out_weight, "mixer_gain": mixer_gain, "up_weight": up_weight, "down_weight": down_weight}


def reference(tokens, queries, keys, values, lambdas, head_gain, out_weight, mixer_gain, up_weight, down_weight):
    query_heads = jnp.transpose(queries.astype(jnp.float32).reshape(TOKENS, HEADS, 2, DQK), (1, 2, 0, 3))
    key_heads = jnp.transpose(keys.astype(jnp.float32).reshape(TOKENS, HEADS, 2, DQK), (1, 2, 0, 3))
    value_heads = jnp.transpose(values.astype(jnp.float32).reshape(TOKENS, HEADS, DV), (1, 0, 2))
    block_rows = math.gcd(TOKENS, 512)
    positions = jnp.arange(TOKENS, dtype=jnp.int32)

    def one_head(inputs):
        query_pair, key_pair, value_rows, lam_value = inputs

        def one_block(block_index):
            offset = (block_index * block_rows).astype(jnp.int32)
            query_pos = offset + jnp.arange(block_rows, dtype=jnp.int32)
            allowed = positions[None, :] <= query_pos[:, None]
            head_maps = []
            for map_index in range(2):
                query_rows = lax.dynamic_slice_in_dim(query_pair[map_index], offset, block_rows, 0)
                scores = jnp.dot(query_rows, key_pair[map_index].T, precision=lax.Precision.HIGHEST, preferred_element_type=jnp.float32) * DQK ** (-0.5)
                scores = jnp.where(allowed, scores, -jnp.inf)
                row_max = lax.optimization_barrier(jnp.max(scores, axis=1, keepdims=True))
                exponent = jnp.exp(scores - row_max)
                row_total = lax.optimization_barrier(jnp.sum(exponent, axis=1, keepdims=True))
                weights = lax.optimization_barrier(exponent.astype(jnp.bfloat16)).astype(jnp.float32)
                head_maps.append(jnp.dot(weights, value_rows, precision=lax.Precision.HIGHEST, preferred_element_type=jnp.float32) / row_total)
            differ = head_maps[0] - lam_value * head_maps[1]
            spread = lax.rsqrt(lax.optimization_barrier(jnp.mean(differ * differ, axis=1, keepdims=True)) + 1e-06)
            return (differ * spread * head_gain).astype(jnp.bfloat16)
        return lax.map(one_block, jnp.arange(TOKENS // block_rows, dtype=jnp.int32))
    attended = lax.map(one_head, (query_heads, key_heads, value_heads, lambdas))
    attended = jnp.transpose(attended.reshape(HEADS, TOKENS, DV), (1, 0, 2)).reshape(TOKENS, HEADS * DV)
    projected = jnp.dot(attended, out_weight, preferred_element_type=jnp.float32).astype(jnp.bfloat16)
    resid = (tokens.astype(jnp.float32) + projected.astype(jnp.float32)).astype(jnp.bfloat16)
    resid_full = resid.astype(jnp.float32)
    normed = (resid_full * lax.rsqrt(lax.optimization_barrier(jnp.mean(resid_full * resid_full, axis=1, keepdims=True)) + 1e-06) * mixer_gain).astype(jnp.bfloat16)
    hidden = jnp.square(jax.nn.relu(jnp.dot(normed, up_weight, preferred_element_type=jnp.float32))).astype(jnp.bfloat16)
    return (resid_full + jnp.dot(hidden, down_weight, preferred_element_type=jnp.float32)).astype(jnp.bfloat16)
```

```python
import functools

import jax
import jax.numpy as jnp
from jax import lax
from jax.experimental import pallas as pl
from jax.experimental.pallas import tpu as pltpu
from jax.sharding import PartitionSpec as P

DQK = 64
MESH = pl.DeviceIdType.MESH
f32, bf16 = jnp.float32, jnp.bfloat16


def front_kernel(
    n, tp,
    lam_ref, q_ref, k_ref, v_ref, gain_ref, up_ref, dn_ref,
    ah_ref, upf_ref, dnf_ref,
    qb, kv, qm, run_max, run_sum, acc, att,
    ex_send, ex_recv, kv_send, kv_recv, w_send, own_send, y_send, w_recv, a_send, a_recv, loc,
):
    s = lax.axis_index("sp")
    t = lax.axis_index("tp")
    z, y = s // 2, lax.rem(s, 2)
    steps = n // 2
    rows = q_ref.shape[0]
    wide = q_ref.shape[1] // 2
    peer = (s + 1 - 2 * y, t)
    above, below = (s + 2, t), (s - 2, t)
    has_up, has_down = z < steps - 1, z > 0
    piece = rows // tp

    barrier = pltpu.get_barrier_semaphore()

    def greet(device):
        pl.semaphore_signal(barrier, inc=1, device_id=device, device_id_type=MESH)

    for e in range(2):
        for i in range(tp):
            who = (2 * z + e, i)

            @pl.when(jnp.logical_or(e != y, i != t))
            def _():
                greet(who)

    pl.when(has_up)(lambda: greet(above))
    pl.when(has_down)(lambda: greet(below))
    pl.semaphore_wait(barrier, 2 * tp - 1 + has_up.astype(jnp.int32) + has_down.astype(jnp.int32))

    def remote(src, dst, send, recv, device):
        return pltpu.make_async_remote_copy(
            src_ref=src, dst_ref=dst, send_sem=send, recv_sem=recv, device_id=device, device_id_type=MESH
        )

    my_rows = pl.ds(pl.multiple_of(y * rows, rows), rows)
    peer_rows = pl.ds(pl.multiple_of((1 - y) * rows, rows), rows)
    my_cols = pl.ds(pl.multiple_of(y * wide, wide), wide)
    peer_cols = pl.ds(pl.multiple_of((1 - y) * wide, wide), wide)
    ex = []
    for i, (src, dst) in enumerate(((k_ref, kv.at[z, 0]), (v_ref, kv.at[z, 1]), (q_ref, qb))):
        ex.append(remote(src.at[:, peer_cols], dst.at[my_rows], ex_send.at[i], ex_recv.at[i], peer))
        ex[-1].start()

    def shard(ref_index, j):
        if ref_index == 0:
            depth = up_ref.shape[0]
            return upf_ref.at[pl.ds(pl.multiple_of(j * depth, depth), depth)]
        return dnf_ref.at[j]

    own = (up_ref, dn_ref)
    for c in range(2):

        @pl.when(has_down)
        def _():
            remote(own[c], shard(c, s), own_send.at[c], w_recv.at[s, c], below).start()

        remote(own[c], shard(c, s), y_send.at[s, c], w_recv.at[s, c], peer).start()
    local = []
    for i, (src, dst) in enumerate(
        (
            (k_ref.at[:, my_cols], kv.at[z, 0, my_rows]),
            (v_ref.at[:, my_cols], kv.at[z, 1, my_rows]),
            (q_ref.at[:, my_cols], qb.at[my_rows]),
            (up_ref, shard(0, s)),
            (dn_ref, shard(1, s)),
        )
    ):
        local.append(pltpu.make_async_copy(src, dst, loc.at[i]))
        local[-1].start()
    for i in range(3):
        local[i].wait()
    for i, (src, dst) in enumerate(((k_ref, kv.at[z, 0]), (v_ref, kv.at[z, 1]), (q_ref, qb))):
        remote(src.at[:, peer_cols], dst.at[peer_rows], ex_send.at[i], ex_recv.at[i], peer).wait_recv()

    def own_up():
        for c in range(2):
            remote(own[c], shard(c, s), w_send.at[s, c], w_recv.at[s, c], above).start()

    def kv_forward(j):
        return remote(kv.at[j], kv.at[j], kv_send.at[j], kv_recv.at[j], above)

    @pl.when(has_up)
    def _():
        kv_forward(z).start()
        pl.when(z == 0)(own_up)

    total = 2 * rows
    lane = lax.broadcasted_iota(jnp.int32, (total, wide), 1)
    scaled = qb[...] * jnp.asarray(DQK ** -0.5, bf16)
    for m in range(2):
        qm[m * total:(m + 1) * total, :] = jnp.where((lane < DQK) == (m == 0), scaled, jnp.zeros_like(scaled))

    chunk = min(256, total)

    def scores_of(r0, j, keys):
        return lax.dot_general(
            qm[pl.ds(r0, chunk), :], kv[j, 0, :keys, :], (((1,), (1,)), ((), ())), preferred_element_type=f32
        )

    for m in range(2):
        for b in range(total // chunk):
            r0, keys = m * total + b * chunk, (b + 1) * chunk
            sc = scores_of(r0, z, keys)
            qpos = b * chunk + lax.broadcasted_iota(jnp.int32, (chunk, keys), 0)
            kpos = lax.broadcasted_iota(jnp.int32, (chunk, keys), 1)
            sc = jnp.where(kpos <= qpos, sc, -jnp.inf)
            top = jnp.max(sc, axis=1, keepdims=True)
            p = jnp.exp(sc - top)
            run_max[pl.ds(r0, chunk), :] = jnp.broadcast_to(top, (chunk, 128))
            run_sum[pl.ds(r0, chunk), :] = jnp.broadcast_to(jnp.sum(p, axis=1, keepdims=True), (chunk, 128))
            acc[pl.ds(r0, chunk), :] = jnp.dot(p.astype(bf16), kv[z, 1, :keys, :], preferred_element_type=f32)

    def block(d, carry):
        j = z - d
        kv_forward(j).wait_recv()

        @pl.when(has_up)
        def _():
            kv_forward(j).start()
            pl.when(j == 0)(own_up)

        def part(b, inner):
            r0 = pl.multiple_of(b * chunk, chunk)
            here = pl.ds(r0, chunk)
            sc = scores_of(r0, j, total)
            old = run_max[here, :]
            top = jnp.maximum(old, jnp.max(sc, axis=1, keepdims=True))
            p = jnp.exp(sc - top[:, :1])
            shrink = jnp.exp(old - top)
            run_max[here, :] = top
            run_sum[here, :] = run_sum[here, :] * shrink + jnp.sum(p, axis=1, keepdims=True)
            acc[here, :] = acc[here, :] * shrink + jnp.dot(p.astype(bf16), kv[j, 1], preferred_element_type=f32)
            return inner

        return lax.fori_loop(0, 2 * total // chunk, part, carry)

    lax.fori_loop(1, z + 1, block, 0)

    lam = lam_ref[y]
    differ = acc[:total, :] / run_sum[:total, :] - lam * (acc[total:, :] / run_sum[total:, :])
    spread = lax.rsqrt(jnp.mean(differ * differ, axis=1, keepdims=True) + 1e-06)
    att[...] = (differ * spread * gain_ref[...]).astype(bf16)

    head = 2 * t + y
    head_cols = pl.ds(pl.multiple_of(head * wide, wide), wide)

    def to_token(e, i, head_index):
        cols = pl.ds(pl.multiple_of(head_index * wide, wide), wide)
        return remote(
            att.at[pl.ds(e * rows + i * piece, piece)], ah_ref.at[:, cols],
            a_send.at[e * tp + i], a_recv.at[head_index], (2 * z + e, i),
        )

    mine = pltpu.make_async_copy(
        att.at[pl.ds(pl.multiple_of(y * rows + t * piece, piece), piece)], ah_ref.at[:, head_cols], loc.at[5]
    )
    mine.start()
    for e in range(2):
        for i in range(tp):
            pl.when(jnp.logical_or(e != y, i != t))(lambda: to_token(e, i, head).start())

    def arrive(j, onward, exists):
        for c in range(2):
            for e in range(1):
                moved = shard(c, j)

                @pl.when(jnp.logical_or(j > s, j < s))
                def _():
                    remote(moved, moved, w_send.at[j, c], w_recv.at[j, c], peer).wait_recv()
                    remote(moved, moved, y_send.at[j, c], w_recv.at[j, c], peer).start()
                    pl.when(exists)(lambda: remote(moved, moved, w_send.at[j, c], w_recv.at[j, c], onward).start())

    def pump(d, carry):
        pl.when(z + d < steps)(lambda: arrive(s + 2 * d, below, has_down))
        pl.when(z - d >= 0)(lambda: arrive(s - 2 * d, above, has_up))
        return carry

    lax.fori_loop(1, steps, pump, 0)

    def across(i, carry):
        j = 2 * i + 1 - y
        for c in range(2):
            remote(shard(c, j), shard(c, j), y_send.at[j, c], w_recv.at[j, c], peer).wait_recv()
        return carry

    lax.fori_loop(0, steps, across, 0)
    for i in range(2 * tp):
        e, who = i % 2, i // 2
        pl.when(jnp.logical_or(e != y, who != t))(lambda: to_token(0, 0, i).wait_recv())

    mine.wait()
    local[3].wait()
    local[4].wait()
    for copy in ex:
        copy.wait_send()
    for e in range(2):
        for i in range(tp):
            pl.when(jnp.logical_or(e != y, i != t))(lambda: to_token(e, i, head).wait_send())

    @pl.when(has_up)
    def _():
        def sent(j, carry):
            kv_forward(j).wait_send()
            return carry

        lax.fori_loop(0, z + 1, sent, 0)

    def line_sent(i, carry):
        j = 2 * i + y
        for c in range(2):
            moved = shard(c, j)
            remote(moved, moved, y_send.at[j, c], w_recv.at[j, c], peer).wait_send()
            gone = jnp.logical_or(jnp.logical_and(i <= z, has_up), jnp.logical_and(i > z, has_down))
            pl.when(gone)(lambda: remote(moved, moved, w_send.at[j, c], w_recv.at[j, c], peer).wait_send())
        return carry

    lax.fori_loop(0, steps, line_sent, 0)

    @pl.when(has_down)
    def _():
        for c in range(2):
            remote(own[c], shard(c, s), own_send.at[c], w_recv.at[s, c], below).wait_send()


def front(n, tp, lambdas, queries, keys, values, head_gain, up_weight, down_weight):
    rows, wide = queries.shape[0], queries.shape[1] // 2
    depth, hid = up_weight.shape
    cols = down_weight.shape[1]
    vmem = pl.BlockSpec(memory_space=pltpu.VMEM)
    dma = pltpu.SemaphoreType.DMA
    return pl.pallas_call(
        functools.partial(front_kernel, n, tp),
        out_shape=(
            jax.ShapeDtypeStruct((rows // tp, 2 * tp * wide), bf16),
            jax.ShapeDtypeStruct((n * depth, hid), bf16),
            jax.ShapeDtypeStruct((n, hid, cols), bf16),
        ),
        in_specs=[pl.BlockSpec(memory_space=pltpu.SMEM)] + [vmem] * 6,
        out_specs=(vmem, vmem, vmem),
        scratch_shapes=[
            pltpu.VMEM((2 * rows, wide), bf16),
            pltpu.VMEM((n // 2, 2, 2 * rows, wide), bf16),
            pltpu.VMEM((4 * rows, wide), bf16),
            pltpu.VMEM((4 * rows, 128), f32),
            pltpu.VMEM((4 * rows, 128), f32),
            pltpu.VMEM((4 * rows, wide), f32),
            pltpu.VMEM((2 * rows, wide), bf16),
            dma((3,)), dma((3,)), dma((n // 2,)), dma((n // 2,)),
            dma((n, 2)), dma((2,)), dma((n, 2)), dma((n, 2)), dma((2 * tp,)), dma((2 * tp,)), dma((6,)),
        ],
        compiler_params=pltpu.CompilerParams(
            collective_id=0, has_side_effects=True, vmem_limit_bytes=60 * 1024 * 1024
        ),
    )(lambdas, queries, keys, values, head_gain.reshape(1, -1), up_weight, down_weight)


def per_device(
    n, tp, tokens, queries, keys, values, lambdas, head_gain, out_weight, mixer_gain, up_weight, down_weight
):
    all_heads, up_full, down_full = front(
        n, tp, lambdas, queries, keys, values, head_gain, up_weight, down_weight
    )
    down_full = jnp.transpose(down_full, (1, 0, 2)).reshape(down_full.shape[1], -1)
    projected = jnp.dot(all_heads, out_weight, preferred_element_type=f32).astype(bf16)
    resid = (tokens.astype(f32) + projected.astype(f32)).astype(bf16)
    resid_full = resid.astype(f32)
    normed = (
        resid_full
        * lax.rsqrt(jnp.mean(resid_full * resid_full, axis=1, keepdims=True) + 1e-06)
        * mixer_gain
    ).astype(bf16)
    hidden = jnp.square(
        jax.nn.relu(
            jnp.dot(lax.all_gather(normed, "tp", axis=0, tiled=True), up_full, preferred_element_type=f32)
        )
    ).astype(bf16)
    mixed = lax.psum_scatter(
        jnp.dot(hidden, down_full, preferred_element_type=f32).astype(bf16),
        "tp",
        scatter_dimension=0,
        tiled=True,
    ).astype(f32)
    return (resid_full + mixed).astype(bf16)


def solution(mesh):
    placed = (
        P(("sp", "tp"), None),
        P("sp", "tp"),
        P("sp", "tp"),
        P("sp", "tp"),
        P("tp"),
        P(),
        P(),
        P(),
        P("sp", "tp"),
        P("tp", "sp"),
    )
    return jax.shard_map(
        functools.partial(per_device, mesh.shape["sp"], mesh.shape["tp"]),
        mesh=mesh,
        in_specs=placed,
        out_specs=P(("sp", "tp"), None),
        check_vma=False,
    )
```

```python
import functools

import jax
import jax.numpy as jnp
from jax import lax
from jax.experimental import pallas as pl
from jax.experimental.pallas import tpu as pltpu
from jax.sharding import PartitionSpec as P

DQK = 64
MESH = pl.DeviceIdType.MESH
f32, bf16 = jnp.float32, jnp.bfloat16


def layer_kernel(
    n, tp,
    lam_ref, q_ref, k_ref, v_ref, gain_ref, up_ref, dn_ref, tok_ref, mix_ref, ow_hbm,
    out_ref,
    ah_ref, upf_ref, dnf_ref,
    qb, kv, qm, run_max, run_sum, acc, att, ow, resid, normed, hsum, hid, part, core_in, cross, cross_in,
    ex_send, ex_recv, kv_send, kv_recv, w_send, own_send, y_send, w_recv, a_send, a_recv, loc,
    ag_send, ag_recv, c_send, c_recv, x_send, x_recv,
):
    s = lax.axis_index("sp")
    t = lax.axis_index("tp")
    z, y = s // 2, lax.rem(s, 2)
    steps = n // 2
    rows = q_ref.shape[0]
    wide = q_ref.shape[1] // 2
    peer = (s + 1 - 2 * y, t)
    above, below = (s + 2, t), (s - 2, t)
    has_up, has_down = z < steps - 1, z > 0
    piece = rows // tp

    barrier = pltpu.get_barrier_semaphore()

    def greet(device):
        pl.semaphore_signal(barrier, inc=1, device_id=device, device_id_type=MESH)

    for e in range(2):
        for i in range(tp):
            who = (2 * z + e, i)

            @pl.when(jnp.logical_or(e != y, i != t))
            def _():
                greet(who)

    pl.when(has_up)(lambda: greet(above))
    pl.when(has_down)(lambda: greet(below))
    pl.semaphore_wait(barrier, 2 * tp - 1 + has_up.astype(jnp.int32) + has_down.astype(jnp.int32))

    def remote(src, dst, send, recv, device):
        return pltpu.make_async_remote_copy(
            src_ref=src, dst_ref=dst, send_sem=send, recv_sem=recv, device_id=device, device_id_type=MESH
        )

    my_rows = pl.ds(pl.multiple_of(y * rows, rows), rows)
    peer_rows = pl.ds(pl.multiple_of((1 - y) * rows, rows), rows)
    my_cols = pl.ds(pl.multiple_of(y * wide, wide), wide)
    peer_cols = pl.ds(pl.multiple_of((1 - y) * wide, wide), wide)
    ex = []
    for i, (src, dst) in enumerate(((k_ref, kv.at[z, 0]), (v_ref, kv.at[z, 1]), (q_ref, qb))):
        ex.append(remote(src.at[:, peer_cols], dst.at[my_rows], ex_send.at[i], ex_recv.at[i], peer))
        ex[-1].start()

    def shard(ref_index, j):
        if ref_index == 0:
            depth = up_ref.shape[0]
            return upf_ref.at[pl.ds(pl.multiple_of(j * depth, depth), depth)]
        return dnf_ref.at[j]

    own = (up_ref, dn_ref)
    for c in range(2):

        @pl.when(has_down)
        def _():
            remote(own[c], shard(c, s), own_send.at[c], w_recv.at[s, c], below).start()

        remote(own[c], shard(c, s), y_send.at[s, c], w_recv.at[s, c], peer).start()
    local = []
    for i, (src, dst) in enumerate(
        (
            (k_ref.at[:, my_cols], kv.at[z, 0, my_rows]),
            (v_ref.at[:, my_cols], kv.at[z, 1, my_rows]),
            (q_ref.at[:, my_cols], qb.at[my_rows]),
            (up_ref, shard(0, s)),
            (dn_ref, shard(1, s)),
            (ow_hbm, ow),
        )
    ):
        local.append(pltpu.make_async_copy(src, dst, loc.at[i]))
        local[-1].start()
    for i in range(3):
        local[i].wait()
    for i, (src, dst) in enumerate(((k_ref, kv.at[z, 0]), (v_ref, kv.at[z, 1]), (q_ref, qb))):
        remote(src.at[:, peer_cols], dst.at[peer_rows], ex_send.at[i], ex_recv.at[i], peer).wait_recv()

    def own_up(c):
        remote(own[c], shard(c, s), w_send.at[s, c], w_recv.at[s, c], above).start()

    def arrive(c, j, onward, exists):
        moved = shard(c, j)
        remote(moved, moved, w_send.at[j, c], w_recv.at[j, c], peer).wait_recv()
        pl.when(exists)(lambda: remote(moved, moved, w_send.at[j, c], w_recv.at[j, c], onward).start())
        remote(moved, moved, y_send.at[j, c], w_recv.at[j, c], peer).start()

    def from_above(d):
        for c in range(2):
            pl.when(z + d < steps)(lambda: arrive(c, s + 2 * d, below, has_down))

    def kv_forward(j):
        return remote(kv.at[j], kv.at[j], kv_send.at[j], kv_recv.at[j], above)

    @pl.when(has_up)
    def _():
        kv_forward(z).start()
        pl.when(z == 0)(lambda: (own_up(0), own_up(1)) and None)

    total = 2 * rows
    lane = lax.broadcasted_iota(jnp.int32, (total, wide), 1)
    scaled = qb[...] * jnp.asarray(DQK ** -0.5, bf16)
    for m in range(2):
        qm[m * total:(m + 1) * total, :] = jnp.where((lane < DQK) == (m == 0), scaled, jnp.zeros_like(scaled))

    chunk = min(256, total)

    def scores_of(r0, j, keys):
        return lax.dot_general(
            qm[pl.ds(r0, chunk), :], kv[j, 0, :keys, :], (((1,), (1,)), ((), ())), preferred_element_type=f32
        )

    for m in range(2):
        for b in range(total // chunk):
            r0, keys = m * total + b * chunk, (b + 1) * chunk
            sc = scores_of(r0, z, keys)
            qpos = b * chunk + lax.broadcasted_iota(jnp.int32, (chunk, keys), 0)
            kpos = lax.broadcasted_iota(jnp.int32, (chunk, keys), 1)
            sc = jnp.where(kpos <= qpos, sc, -jnp.inf)
            top = jnp.max(sc, axis=1, keepdims=True)
            p = jnp.exp(sc - top)
            run_max[pl.ds(r0, chunk), :] = jnp.broadcast_to(top, (chunk, 128))
            run_sum[pl.ds(r0, chunk), :] = jnp.broadcast_to(jnp.sum(p, axis=1, keepdims=True), (chunk, 128))
            acc[pl.ds(r0, chunk), :] = jnp.dot(p.astype(bf16), kv[z, 1, :keys, :], preferred_element_type=f32)

    def block(d, carry):
        j = z - d
        kv_forward(j).wait_recv()

        @pl.when(has_up)
        def _():
            kv_forward(j).start()
            pl.when(j == 0)(lambda: own_up(0))

        def tile(b, inner):
            r0 = pl.multiple_of(b * chunk, chunk)
            here = pl.ds(r0, chunk)
            sc = scores_of(r0, j, total)
            old = run_max[here, :]
            top = jnp.maximum(old, jnp.max(sc, axis=1, keepdims=True))
            p = jnp.exp(sc - top[:, :1])
            shrink = jnp.exp(old - top)
            run_max[here, :] = top
            run_sum[here, :] = run_sum[here, :] * shrink + jnp.sum(p, axis=1, keepdims=True)
            acc[here, :] = acc[here, :] * shrink + jnp.dot(p.astype(bf16), kv[j, 1], preferred_element_type=f32)
            return inner

        lax.fori_loop(0, 2 * total // chunk, tile, 0)
        pl.when(d == 1)(lambda: from_above(1))
        return carry

    lax.fori_loop(1, z + 1, block, 0)

    lam = lam_ref[y]
    differ = acc[:total, :] / run_sum[:total, :] - lam * (acc[total:, :] / run_sum[total:, :])
    spread = lax.rsqrt(jnp.mean(differ * differ, axis=1, keepdims=True) + 1e-06)
    att[...] = (differ * spread * gain_ref[...]).astype(bf16)

    head = 2 * t + y
    head_cols = pl.ds(pl.multiple_of(head * wide, wide), wide)

    def to_token(e, i, head_index):
        cols = pl.ds(pl.multiple_of(head_index * wide, wide), wide)
        return remote(
            att.at[pl.ds(e * rows + i * piece, piece)], ah_ref.at[:, cols],
            a_send.at[e * tp + i], a_recv.at[head_index], (2 * z + e, i),
        )

    mine = pltpu.make_async_copy(
        att.at[pl.ds(pl.multiple_of(y * rows + t * piece, piece), piece)], ah_ref.at[:, head_cols], loc.at[6]
    )
    mine.start()
    for e in range(2):
        for i in range(tp):
            pl.when(jnp.logical_or(e != y, i != t))(lambda: to_token(e, i, head).start())

    def from_below(c, d):
        @pl.when(z - d >= 0)
        def _():
            arrive(c, s - 2 * d, above, has_up)
            if c == 0:
                pl.when(jnp.logical_and(d == z, has_up))(lambda: own_up(1))

    pl.when(z == 0)(lambda: from_above(1))
    local[5].wait()
    mine.wait()
    for i in range(2 * tp):
        e, who = i % 2, i // 2
        pl.when(jnp.logical_or(e != y, who != t))(lambda: to_token(0, 0, i).wait_recv())

    projected = jnp.dot(ah_ref[...], ow[...], preferred_element_type=f32).astype(bf16)
    summed = (tok_ref[...].astype(f32) + projected.astype(f32)).astype(bf16)
    resid[...] = summed
    summed = summed.astype(f32)
    scale = lax.rsqrt(jnp.mean(summed * summed, axis=1, keepdims=True) + 1e-06)

    tc = t + 1 - 2 * lax.rem(t, 2)
    tx = lax.rem(t + 2, tp)
    td = lax.rem(tc + 2, tp)

    def band(i):
        return pl.ds(pl.multiple_of(i * piece, piece), piece)

    normed[band(t), :] = (summed * scale * mix_ref[...]).astype(bf16)

    def gathered(k, block_index, device):
        block_ref = normed.at[band(block_index)]
        return remote(block_ref, block_ref, ag_send.at[k], ag_recv.at[block_index], (s, device))

    gathered(0, t, tx).start()
    gathered(1, t, tc).start()

    def pump(d, carry):
        from_below(0, d)
        pl.when(d > 1)(lambda: from_above(d))
        return carry

    lax.fori_loop(1, min(3, steps), pump, 0)
    gathered(0, tx, tx).wait_recv()
    gathered(2, tx, tc).start()
    lax.fori_loop(min(3, steps), steps, pump, 0)
    gathered(1, tc, tc).wait_recv()
    gathered(2, td, tc).wait_recv()
    local[3].wait()
    local[4].wait()

    def order(k):
        return jnp.where(k < steps - z, z + k, steps - 1 - k)

    def across(c, i):
        j = 2 * i + 1 - y
        remote(shard(c, j), shard(c, j), y_send.at[j, c], w_recv.at[j, c], peer).wait_recv()

    pair_depth = 2 * up_ref.shape[0]
    hsum[...] = jnp.zeros_like(hsum)

    def up_pair(k, carry):
        i = order(k)
        across(0, i)
        span = pl.ds(pl.multiple_of(i * pair_depth, pair_depth), pair_depth)
        hsum[...] += jnp.dot(normed[:, span], upf_ref[span, :], preferred_element_type=f32)
        return carry

    lax.fori_loop(0, steps, up_pair, 0)
    hid[...] = jnp.square(jnp.maximum(hsum[...], 0.0)).astype(bf16)

    def to_core(j, m):
        return remote(
            part.at[j, band(tc if m == 0 else td)], core_in.at[j, m], c_send.at[j, m], c_recv.at[j, m], (s, tc)
        )

    def to_cross(j):
        return remote(cross.at[j], cross_in.at[j], x_send.at[j], x_recv.at[j], (s, tx))

    def add_cores(i):
        for e in range(2):
            j = 2 * i + e
            to_core(j, 1).wait_recv()
            cross[j] = (part[j, band(tx), :].astype(f32) + core_in[j, 1].astype(f32)).astype(bf16)
            to_cross(j).start()

    def down_pair(k, carry):
        i = order(k)
        later = order(k + 1)

        @pl.when(jnp.logical_and(k + 1 < steps, later < z))
        def _():
            arrive(1, 2 * later + y, above, has_up)

        across(1, i)
        for e in range(2):
            j = 2 * i + e
            part[j] = jnp.dot(hid[...], dnf_ref[j], preferred_element_type=f32).astype(bf16)
            to_core(j, 1).start()
            to_core(j, 0).start()
        pl.when(k > 0)(lambda: add_cores(order(k - 1)))
        return carry

    lax.fori_loop(0, steps, down_pair, 0)
    add_cores(order(steps - 1))

    cols = dn_ref.shape[1]
    for j in range(n):
        to_core(j, 0).wait_recv()
        to_cross(j).wait_recv()
        here = slice(j * cols, (j + 1) * cols)
        both = part[j, band(t), :].astype(f32) + core_in[j, 0].astype(f32) + cross_in[j].astype(f32)
        out_ref[:, here] = (resid[:, here].astype(f32) + both).astype(bf16)

    gathered(0, t, tx).wait_send()
    gathered(1, t, tc).wait_send()
    gathered(2, tx, tc).wait_send()
    for j in range(n):
        to_core(j, 0).wait_send()
        to_core(j, 1).wait_send()
        to_cross(j).wait_send()
    for copy in ex:
        copy.wait_send()
    for e in range(2):
        for i in range(tp):
            pl.when(jnp.logical_or(e != y, i != t))(lambda: to_token(e, i, head).wait_send())

    @pl.when(has_up)
    def _():
        def sent(j, carry):
            kv_forward(j).wait_send()
            return carry

        lax.fori_loop(0, z + 1, sent, 0)

    def line_sent(i, carry):
        j = 2 * i + y
        for c in range(2):
            moved = shard(c, j)
            remote(moved, moved, y_send.at[j, c], w_recv.at[j, c], peer).wait_send()
            gone = jnp.logical_or(jnp.logical_and(i <= z, has_up), jnp.logical_and(i > z, has_down))
            pl.when(gone)(lambda: remote(moved, moved, w_send.at[j, c], w_recv.at[j, c], peer).wait_send())
        return carry

    lax.fori_loop(0, steps, line_sent, 0)

    @pl.when(has_down)
    def _():
        for c in range(2):
            remote(own[c], shard(c, s), own_send.at[c], w_recv.at[s, c], below).wait_send()


def per_device(
    n, tp, tokens, queries, keys, values, lambdas, head_gain, out_weight, mixer_gain, up_weight, down_weight
):
    rows, wide = queries.shape[0], queries.shape[1] // 2
    depth, units = up_weight.shape
    cols = down_weight.shape[1]
    piece, width = tokens.shape
    vmem = pl.BlockSpec(memory_space=pltpu.VMEM)
    dma = pltpu.SemaphoreType.DMA
    return pl.pallas_call(
        functools.partial(layer_kernel, n, tp),
        out_shape=jax.ShapeDtypeStruct(tokens.shape, bf16),
        in_specs=[pl.BlockSpec(memory_space=pltpu.SMEM)] + [vmem] * 8 + [pl.BlockSpec(memory_space=pl.ANY)],
        out_specs=vmem,
        scratch_shapes=[
            pltpu.VMEM((piece, 2 * tp * wide), bf16),
            pltpu.VMEM((n * depth, units), bf16),
            pltpu.VMEM((n, units, cols), bf16),
            pltpu.VMEM((2 * rows, wide), bf16),
            pltpu.VMEM((n // 2, 2, 2 * rows, wide), bf16),
            pltpu.VMEM((4 * rows, wide), bf16),
            pltpu.VMEM((4 * rows, 128), f32),
            pltpu.VMEM((4 * rows, 128), f32),
            pltpu.VMEM((4 * rows, wide), f32),
            pltpu.VMEM((2 * rows, wide), bf16),
            pltpu.VMEM(out_weight.shape, bf16),
            pltpu.VMEM((piece, width), bf16),
            pltpu.VMEM((rows, width), bf16),
            pltpu.VMEM((rows, units), f32),
            pltpu.VMEM((rows, units), bf16),
            pltpu.VMEM((n, rows, cols), bf16),
            pltpu.VMEM((n, 2, piece, cols), bf16),
            pltpu.VMEM((n, piece, cols), bf16),
            pltpu.VMEM((n, piece, cols), bf16),
            dma((3,)), dma((3,)), dma((n // 2,)), dma((n // 2,)),
            dma((n, 2)), dma((2,)), dma((n, 2)), dma((n, 2)), dma((2 * tp,)), dma((2 * tp,)), dma((7,)),
            dma((3,)), dma((tp,)), dma((n, 2)), dma((n, 2)), dma((n,)), dma((n,)),
        ],
        compiler_params=pltpu.CompilerParams(
            collective_id=0, has_side_effects=True, vmem_limit_bytes=60 * 1024 * 1024
        ),
    )(
        lambdas, queries, keys, values, head_gain.reshape(1, -1), up_weight, down_weight,
        tokens, mixer_gain.reshape(1, -1), out_weight,
    )


def solution(mesh):
    placed = (
        P(("sp", "tp"), None),
        P("sp", "tp"),
        P("sp", "tp"),
        P("sp", "tp"),
        P("tp"),
        P(),
        P(),
        P(),
        P("sp", "tp"),
        P("tp", "sp"),
    )
    return jax.shard_map(
        functools.partial(per_device, mesh.shape["sp"], mesh.shape["tp"]),
        mesh=mesh,
        in_specs=placed,
        out_specs=P(("sp", "tp"), None),
        check_vma=False,
    )
```

```python
import functools

import jax
import jax.numpy as jnp
from jax import lax
from jax.experimental import pallas as pl
from jax.experimental.pallas import tpu as pltpu
from jax.sharding import PartitionSpec as P

DQK = 64
MESH = pl.DeviceIdType.MESH
f32, bf16 = jnp.float32, jnp.bfloat16


def layer_kernel(
    n, tp,
    lam_ref, q_ref, k_ref, v_ref, gain_ref, up_ref, dn_ref, tok_ref, mix_ref, ow_hbm,
    out_ref,
    ah_ref, upf_ref, dnf_ref,
    qb, kv, qm, run_max, run_sum, acc, att, ow, resid, normed, hsum, hid, part, core_in, cross, cross_in,
    ex_send, ex_recv, kv_send, kv_recv, w_send, own_send, y_send, w_recv, a_send, a_recv, loc,
    ag_send, ag_recv, c_send, c_recv, x_send, x_recv,
):
    s = lax.axis_index("sp")
    t = lax.axis_index("tp")
    z, y = s // 2, lax.rem(s, 2)
    steps = n // 2
    rows = q_ref.shape[0]
    wide = q_ref.shape[1] // 2
    peer = (s + 1 - 2 * y, t)
    above, below = (s + 2, t), (s - 2, t)
    has_up, has_down = z < steps - 1, z > 0
    piece = rows // tp

    barrier = pltpu.get_barrier_semaphore()

    def greet(device):
        pl.semaphore_signal(barrier, inc=1, device_id=device, device_id_type=MESH)

    for e in range(2):
        for i in range(tp):
            who = (2 * z + e, i)

            @pl.when(jnp.logical_or(e != y, i != t))
            def _():
                greet(who)

    pl.when(has_up)(lambda: greet(above))
    pl.when(has_down)(lambda: greet(below))
    pl.semaphore_wait(barrier, 2 * tp - 1 + has_up.astype(jnp.int32) + has_down.astype(jnp.int32))

    def remote(src, dst, send, recv, device):
        return pltpu.make_async_remote_copy(
            src_ref=src, dst_ref=dst, send_sem=send, recv_sem=recv, device_id=device, device_id_type=MESH
        )

    my_rows = pl.ds(pl.multiple_of(y * rows, rows), rows)
    peer_rows = pl.ds(pl.multiple_of((1 - y) * rows, rows), rows)
    my_cols = pl.ds(pl.multiple_of(y * wide, wide), wide)
    peer_cols = pl.ds(pl.multiple_of((1 - y) * wide, wide), wide)
    ex = []
    for i, (src, dst) in enumerate(((k_ref, kv.at[z, 0]), (v_ref, kv.at[z, 1]), (q_ref, qb))):
        ex.append(remote(src.at[:, peer_cols], dst.at[my_rows], ex_send.at[i], ex_recv.at[i], peer))
        ex[-1].start()

    half = dn_ref.shape[0] // 2
    halves = (slice(0, half), slice(half, 2 * half))

    def shard(c, j):
        if c == 0:
            depth = up_ref.shape[0]
            return upf_ref.at[pl.ds(pl.multiple_of(j * depth, depth), depth)]
        return dnf_ref.at[j, halves[c - 1]]

    own = (up_ref, dn_ref.at[halves[0]], dn_ref.at[halves[1]])

    def own_up(c):
        remote(own[c], shard(c, s), w_send.at[s, c], w_recv.at[s, c], above).start()

    pl.when(has_up)(lambda: own_up(0))
    for c in range(3):

        @pl.when(has_down)
        def _():
            remote(own[c], shard(c, s), own_send.at[c], w_recv.at[s, c], below).start()

        remote(own[c], shard(c, s), y_send.at[s, c], w_recv.at[s, c], peer).start()
    local = []
    for i, (src, dst) in enumerate(
        (
            (k_ref.at[:, my_cols], kv.at[z, 0, my_rows]),
            (v_ref.at[:, my_cols], kv.at[z, 1, my_rows]),
            (q_ref.at[:, my_cols], qb.at[my_rows]),
            (up_ref, shard(0, s)),
            (dn_ref, dnf_ref.at[s]),
            (ow_hbm, ow),
        )
    ):
        local.append(pltpu.make_async_copy(src, dst, loc.at[i]))
        local[-1].start()
    for i in range(3):
        local[i].wait()
    for i, (src, dst) in enumerate(((k_ref, kv.at[z, 0]), (v_ref, kv.at[z, 1]), (q_ref, qb))):
        remote(src.at[:, peer_cols], dst.at[peer_rows], ex_send.at[i], ex_recv.at[i], peer).wait_recv()

    def onward(c, j, device):
        moved = shard(c, j)
        remote(moved, moved, w_send.at[j, c], w_recv.at[j, c], device).start()

    def landed(c, j):
        moved = shard(c, j)
        remote(moved, moved, w_send.at[j, c], w_recv.at[j, c], peer).wait_recv()
        remote(moved, moved, y_send.at[j, c], w_recv.at[j, c], peer).start()

    def arrive(c, j, device, exists):
        landed(c, j)
        pl.when(exists)(lambda: onward(c, j, device))

    def down_up():
        own_up(1)
        own_up(2)

    def from_above(d):
        for c in range(3):
            pl.when(z + d < steps)(lambda: arrive(c, s + 2 * d, below, has_down))

    def kv_forward(j):
        return remote(kv.at[j], kv.at[j], kv_send.at[j], kv_recv.at[j], above)

    @pl.when(has_up)
    def _():
        kv_forward(z).start()
        pl.when(z == 0)(down_up)

    total = 2 * rows
    lane = lax.broadcasted_iota(jnp.int32, (total, wide), 1)
    scaled = qb[...] * jnp.asarray(DQK ** -0.5, bf16)
    for m in range(2):
        qm[m * total:(m + 1) * total, :] = jnp.where((lane < DQK) == (m == 0), scaled, jnp.zeros_like(scaled))

    chunk = min(256, total)

    def scores_of(r0, j, keys):
        return lax.dot_general(
            qm[pl.ds(r0, chunk), :], kv[j, 0, :keys, :], (((1,), (1,)), ((), ())), preferred_element_type=f32
        )

    for m in range(2):
        for b in range(total // chunk):
            r0, keys = m * total + b * chunk, (b + 1) * chunk
            sc = scores_of(r0, z, keys)
            qpos = b * chunk + lax.broadcasted_iota(jnp.int32, (chunk, keys), 0)
            kpos = lax.broadcasted_iota(jnp.int32, (chunk, keys), 1)
            sc = jnp.where(kpos <= qpos, sc, -jnp.inf)
            top = jnp.max(sc, axis=1, keepdims=True)
            p = jnp.exp(sc - top)
            run_max[pl.ds(r0, chunk), :] = jnp.broadcast_to(top, (chunk, 128))
            run_sum[pl.ds(r0, chunk), :] = jnp.broadcast_to(jnp.sum(p, axis=1, keepdims=True), (chunk, 128))
            acc[pl.ds(r0, chunk), :] = jnp.dot(p.astype(bf16), kv[z, 1, :keys, :], preferred_element_type=f32)

    def block(d, carry):
        j = z - d
        pl.when(d == 1)(lambda: landed(0, s - 2))
        kv_forward(j).wait_recv()

        @pl.when(has_up)
        def _():
            kv_forward(j).start()

            @pl.when(j == 0)
            def _():
                onward(0, s - 2, above)
                pl.when(z == 1)(down_up)

        def tile(b, inner):
            r0 = pl.multiple_of(b * chunk, chunk)
            here = pl.ds(r0, chunk)
            sc = scores_of(r0, j, total)
            old = run_max[here, :]
            top = jnp.maximum(old, jnp.max(sc, axis=1, keepdims=True))
            p = jnp.exp(sc - top[:, :1])
            shrink = jnp.exp(old - top)
            run_max[here, :] = top
            run_sum[here, :] = run_sum[here, :] * shrink + jnp.sum(p, axis=1, keepdims=True)
            acc[here, :] = acc[here, :] * shrink + jnp.dot(p.astype(bf16), kv[j, 1], preferred_element_type=f32)
            return inner

        lax.fori_loop(0, 2 * total // chunk, tile, 0)
        pl.when(d == 1)(lambda: from_above(1))
        return carry

    lax.fori_loop(1, z + 1, block, 0)

    lam = lam_ref[y]
    differ = acc[:total, :] / run_sum[:total, :] - lam * (acc[total:, :] / run_sum[total:, :])
    spread = lax.rsqrt(jnp.mean(differ * differ, axis=1, keepdims=True) + 1e-06)
    att[...] = (differ * spread * gain_ref[...]).astype(bf16)

    head = 2 * t + y
    head_cols = pl.ds(pl.multiple_of(head * wide, wide), wide)

    def to_token(e, i, head_index):
        cols = pl.ds(pl.multiple_of(head_index * wide, wide), wide)
        return remote(
            att.at[pl.ds(e * rows + i * piece, piece)], ah_ref.at[:, cols],
            a_send.at[e * tp + i], a_recv.at[head_index], (2 * z + e, i),
        )

    mine = pltpu.make_async_copy(
        att.at[pl.ds(pl.multiple_of(y * rows + t * piece, piece), piece)], ah_ref.at[:, head_cols], loc.at[6]
    )
    mine.start()
    for e in range(2):
        for i in range(tp):
            pl.when(jnp.logical_or(e != y, i != t))(lambda: to_token(e, i, head).start())

    def up_below(d):
        @pl.when(z - d >= 0)
        def _():
            arrive(0, s - 2 * d, above, has_up)
            pl.when(jnp.logical_and(d == z, has_up))(down_up)

    pl.when(z == 0)(lambda: from_above(1))
    local[5].wait()
    mine.wait()
    for i in range(2 * tp):
        e, who = i % 2, i // 2
        pl.when(jnp.logical_or(e != y, who != t))(lambda: to_token(0, 0, i).wait_recv())

    projected = jnp.dot(ah_ref[...], ow[...], preferred_element_type=f32).astype(bf16)
    summed = (tok_ref[...].astype(f32) + projected.astype(f32)).astype(bf16)
    resid[...] = summed
    summed = summed.astype(f32)
    scale = lax.rsqrt(jnp.mean(summed * summed, axis=1, keepdims=True) + 1e-06)

    tc = t + 1 - 2 * lax.rem(t, 2)
    tx = lax.rem(t + 2, tp)
    td = lax.rem(tc + 2, tp)

    def band(i):
        return pl.ds(pl.multiple_of(i * piece, piece), piece)

    normed[band(t), :] = (summed * scale * mix_ref[...]).astype(bf16)

    def gathered(k, block_index, device):
        block_ref = normed.at[band(block_index)]
        return remote(block_ref, block_ref, ag_send.at[k], ag_recv.at[block_index], (s, device))

    gathered(0, t, tx).start()
    gathered(1, t, tc).start()

    def pump(d, carry):
        up_below(d)
        from_above(d)
        return carry

    lax.fori_loop(2, min(3, steps), pump, 0)
    gathered(0, tx, tx).wait_recv()
    gathered(2, tx, tc).start()
    lax.fori_loop(min(3, steps), steps, pump, 0)
    gathered(1, tc, tc).wait_recv()
    gathered(2, td, tc).wait_recv()
    local[3].wait()
    local[4].wait()

    def order(k):
        return jnp.where(k < steps - z, z + k, steps - 1 - k)

    def across(c, i):
        j = 2 * i + 1 - y
        remote(shard(c, j), shard(c, j), y_send.at[j, c], w_recv.at[j, c], peer).wait_recv()

    pair_depth = 2 * up_ref.shape[0]
    hsum[...] = jnp.zeros_like(hsum)

    def up_pair(k, carry):
        i = order(k)
        across(0, i)
        span = pl.ds(pl.multiple_of(i * pair_depth, pair_depth), pair_depth)
        hsum[...] += jnp.dot(normed[:, span], upf_ref[span, :], preferred_element_type=f32)
        return carry

    lax.fori_loop(0, steps, up_pair, 0)
    hid[...] = jnp.square(jnp.maximum(hsum[...], 0.0)).astype(bf16)

    def to_core(j, m):
        return remote(
            part.at[j, band(tc if m == 0 else td)], core_in.at[j, m], c_send.at[j, m], c_recv.at[j, m], (s, tc)
        )

    def to_cross(j):
        return remote(cross.at[j], cross_in.at[j], x_send.at[j], x_recv.at[j], (s, tx))

    def add_cores(i):
        for e in range(2):
            j = 2 * i + e
            to_core(j, 1).wait_recv()
            cross[j] = (part[j, band(tx), :].astype(f32) + core_in[j, 1].astype(f32)).astype(bf16)
            to_cross(j).start()

    def down_pair(k, carry):
        i = order(k)
        later = order(k + 1)

        @pl.when(jnp.logical_and(k + 1 < steps, later < z))
        def _():
            arrive(1, 2 * later + y, above, has_up)
            arrive(2, 2 * later + y, above, has_up)

        pl.when(k > 0)(lambda: add_cores(order(k - 1)))
        across(1, i)
        across(2, i)
        for e in range(2):
            j = 2 * i + e
            part[j] = jnp.dot(hid[...], dnf_ref[j], preferred_element_type=f32).astype(bf16)
            to_core(j, 1).start()
            to_core(j, 0).start()
        return carry

    lax.fori_loop(0, steps, down_pair, 0)
    add_cores(order(steps - 1))

    cols = dn_ref.shape[1]
    for j in range(n):
        to_core(j, 0).wait_recv()
        to_cross(j).wait_recv()
        here = slice(j * cols, (j + 1) * cols)
        both = part[j, band(t), :].astype(f32) + core_in[j, 0].astype(f32) + cross_in[j].astype(f32)
        out_ref[:, here] = (resid[:, here].astype(f32) + both).astype(bf16)

    gathered(0, t, tx).wait_send()
    gathered(1, t, tc).wait_send()
    gathered(2, tx, tc).wait_send()
    for j in range(n):
        to_core(j, 0).wait_send()
        to_core(j, 1).wait_send()
        to_cross(j).wait_send()
    for copy in ex:
        copy.wait_send()
    for e in range(2):
        for i in range(tp):
            pl.when(jnp.logical_or(e != y, i != t))(lambda: to_token(e, i, head).wait_send())

    @pl.when(has_up)
    def _():
        def sent(j, carry):
            kv_forward(j).wait_send()
            return carry

        lax.fori_loop(0, z + 1, sent, 0)

    def line_sent(i, carry):
        j = 2 * i + y
        for c in range(3):
            moved = shard(c, j)
            remote(moved, moved, y_send.at[j, c], w_recv.at[j, c], peer).wait_send()
            gone = jnp.logical_or(jnp.logical_and(i <= z, has_up), jnp.logical_and(i > z, has_down))
            pl.when(gone)(lambda: remote(moved, moved, w_send.at[j, c], w_recv.at[j, c], peer).wait_send())
        return carry

    lax.fori_loop(0, steps, line_sent, 0)

    @pl.when(has_down)
    def _():
        for c in range(3):
            remote(own[c], shard(c, s), own_send.at[c], w_recv.at[s, c], below).wait_send()


def per_device(
    n, tp, tokens, queries, keys, values, lambdas, head_gain, out_weight, mixer_gain, up_weight, down_weight
):
    rows, wide = queries.shape[0], queries.shape[1] // 2
    depth, units = up_weight.shape
    cols = down_weight.shape[1]
    piece, width = tokens.shape
    vmem = pl.BlockSpec(memory_space=pltpu.VMEM)
    dma = pltpu.SemaphoreType.DMA
    return pl.pallas_call(
        functools.partial(layer_kernel, n, tp),
        out_shape=jax.ShapeDtypeStruct(tokens.shape, bf16),
        in_specs=[pl.BlockSpec(memory_space=pltpu.SMEM)] + [vmem] * 8 + [pl.BlockSpec(memory_space=pl.ANY)],
        out_specs=vmem,
        scratch_shapes=[
            pltpu.VMEM((piece, 2 * tp * wide), bf16),
            pltpu.VMEM((n * depth, units), bf16),
            pltpu.VMEM((n, units, cols), bf16),
            pltpu.VMEM((2 * rows, wide), bf16),
            pltpu.VMEM((n // 2, 2, 2 * rows, wide), bf16),
            pltpu.VMEM((4 * rows, wide), bf16),
            pltpu.VMEM((4 * rows, 128), f32),
            pltpu.VMEM((4 * rows, 128), f32),
            pltpu.VMEM((4 * rows, wide), f32),
            pltpu.VMEM((2 * rows, wide), bf16),
            pltpu.VMEM(out_weight.shape, bf16),
            pltpu.VMEM((piece, width), bf16),
            pltpu.VMEM((rows, width), bf16),
            pltpu.VMEM((rows, units), f32),
            pltpu.VMEM((rows, units), bf16),
            pltpu.VMEM((n, rows, cols), bf16),
            pltpu.VMEM((n, 2, piece, cols), bf16),
            pltpu.VMEM((n, piece, cols), bf16),
            pltpu.VMEM((n, piece, cols), bf16),
            dma((3,)), dma((3,)), dma((n // 2,)), dma((n // 2,)),
            dma((n, 3)), dma((3,)), dma((n, 3)), dma((n, 3)), dma((2 * tp,)), dma((2 * tp,)), dma((7,)),
            dma((3,)), dma((tp,)), dma((n, 2)), dma((n, 2)), dma((n,)), dma((n,)),
        ],
        compiler_params=pltpu.CompilerParams(
            collective_id=0, has_side_effects=True, vmem_limit_bytes=60 * 1024 * 1024
        ),
    )(
        lambdas, queries, keys, values, head_gain.reshape(1, -1), up_weight, down_weight,
        tokens, mixer_gain.reshape(1, -1), out_weight,
    )


def solution(mesh):
    placed = (
        P(("sp", "tp"), None),
        P("sp", "tp"),
        P("sp", "tp"),
        P("sp", "tp"),
        P("tp"),
        P(),
        P(),
        P(),
        P("sp", "tp"),
        P("tp", "sp"),
    )
    return jax.shard_map(
        functools.partial(per_device, mesh.shape["sp"], mesh.shape["tp"]),
        mesh=mesh,
        in_specs=placed,
        out_specs=P(("sp", "tp"), None),
        check_vma=False,
    )
```

```python
import functools

import jax
import jax.numpy as jnp
from jax import lax
from jax.experimental import pallas as pl
from jax.experimental.pallas import tpu as pltpu
from jax.sharding import PartitionSpec as P

DQK = 64
MESH = pl.DeviceIdType.MESH
f32, bf16 = jnp.float32, jnp.bfloat16


def layer_kernel(
    n, tp,
    lam_ref, q_ref, k_ref, v_ref, gain_ref, up_ref, dn_ref, tok_ref, mix_ref, ow_hbm,
    out_ref,
    ah_ref, upf_ref, dnf_ref,
    qb, kv, qm, run_max, run_sum, acc, att, ow, resid, normed, hsum, hid, part, core_in, cross, cross_in,
    ex_send, ex_recv, kv_send, kv_recv, w_send, own_send, y_send, w_recv, a_send, a_recv, loc,
    ag_send, ag_recv, c_send, c_recv, x_send, x_recv,
):
    s = lax.axis_index("sp")
    t = lax.axis_index("tp")
    z, y = s // 2, lax.rem(s, 2)
    steps = n // 2
    rows = q_ref.shape[0]
    wide = q_ref.shape[1] // 2
    peer = (s + 1 - 2 * y, t)
    above, below = (s + 2, t), (s - 2, t)
    has_up, has_down = z < steps - 1, z > 0
    piece = rows // tp

    barrier = pltpu.get_barrier_semaphore()

    def greet(device):
        pl.semaphore_signal(barrier, inc=1, device_id=device, device_id_type=MESH)

    for e in range(2):
        for i in range(tp):
            who = (2 * z + e, i)

            @pl.when(jnp.logical_or(e != y, i != t))
            def _():
                greet(who)

    pl.when(has_up)(lambda: greet(above))
    pl.when(has_down)(lambda: greet(below))
    pl.semaphore_wait(barrier, 2 * tp - 1 + has_up.astype(jnp.int32) + has_down.astype(jnp.int32))

    def remote(src, dst, send, recv, device):
        return pltpu.make_async_remote_copy(
            src_ref=src, dst_ref=dst, send_sem=send, recv_sem=recv, device_id=device, device_id_type=MESH
        )

    my_rows = pl.ds(pl.multiple_of(y * rows, rows), rows)
    peer_rows = pl.ds(pl.multiple_of((1 - y) * rows, rows), rows)
    my_cols = pl.ds(pl.multiple_of(y * wide, wide), wide)
    peer_cols = pl.ds(pl.multiple_of((1 - y) * wide, wide), wide)
    ex = []
    for i, (src, dst) in enumerate(((k_ref, kv.at[z, 0]), (v_ref, kv.at[z, 1]), (q_ref, qb))):
        ex.append(remote(src.at[:, peer_cols], dst.at[my_rows], ex_send.at[i], ex_recv.at[i], peer))
        ex[-1].start()

    half = dn_ref.shape[0] // 2
    halves = (slice(0, half), slice(half, 2 * half))

    def shard(c, j):
        if c == 0:
            depth = up_ref.shape[0]
            return upf_ref.at[pl.ds(pl.multiple_of(j * depth, depth), depth)]
        return dnf_ref.at[j, halves[c - 1]]

    own = (up_ref, dn_ref.at[halves[0]], dn_ref.at[halves[1]])

    def own_up(c):
        remote(own[c], shard(c, s), w_send.at[s, c], w_recv.at[s, c], above).start()

    pl.when(has_up)(lambda: own_up(0))
    for c in range(3):

        @pl.when(has_down)
        def _():
            remote(own[c], shard(c, s), own_send.at[c], w_recv.at[s, c], below).start()

        remote(own[c], shard(c, s), y_send.at[s, c], w_recv.at[s, c], peer).start()
    local = []
    for i, (src, dst) in enumerate(
        (
            (k_ref.at[:, my_cols], kv.at[z, 0, my_rows]),
            (v_ref.at[:, my_cols], kv.at[z, 1, my_rows]),
            (q_ref.at[:, my_cols], qb.at[my_rows]),
            (up_ref, shard(0, s)),
            (dn_ref, dnf_ref.at[s]),
            (ow_hbm, ow),
        )
    ):
        local.append(pltpu.make_async_copy(src, dst, loc.at[i]))
        local[-1].start()
    for i in range(3):
        local[i].wait()
    for i, (src, dst) in enumerate(((k_ref, kv.at[z, 0]), (v_ref, kv.at[z, 1]), (q_ref, qb))):
        remote(src.at[:, peer_cols], dst.at[peer_rows], ex_send.at[i], ex_recv.at[i], peer).wait_recv()

    def onward(c, j, device):
        moved = shard(c, j)
        remote(moved, moved, w_send.at[j, c], w_recv.at[j, c], device).start()

    def await_chunk(c, j):
        moved = shard(c, j)
        remote(moved, moved, w_send.at[j, c], w_recv.at[j, c], peer).wait_recv()

    def over(c, j):
        moved = shard(c, j)
        remote(moved, moved, y_send.at[j, c], w_recv.at[j, c], peer).start()

    def arrive(c, j, device, exists):
        await_chunk(c, j)
        over(c, j)
        pl.when(exists)(lambda: onward(c, j, device))

    def next_above(c):
        @pl.when(z + 1 < steps)
        def _():
            await_chunk(c, s + 2)
            pl.when(has_down)(lambda: onward(c, s + 2, below))

    def down_up():
        own_up(1)
        own_up(2)

    def from_above(d):
        for c in range(3):
            pl.when(z + d < steps)(lambda: arrive(c, s + 2 * d, below, has_down))

    def kv_forward(j):
        return remote(kv.at[j], kv.at[j], kv_send.at[j], kv_recv.at[j], above)

    @pl.when(has_up)
    def _():
        kv_forward(z).start()
        pl.when(z == 0)(down_up)

    total = 2 * rows
    lane = lax.broadcasted_iota(jnp.int32, (total, wide), 1)
    scaled = qb[...] * jnp.asarray(DQK ** -0.5, bf16)
    for m in range(2):
        qm[m * total:(m + 1) * total, :] = jnp.where((lane < DQK) == (m == 0), scaled, jnp.zeros_like(scaled))

    chunk = min(256, total)

    def scores_of(r0, j, keys):
        return lax.dot_general(
            qm[pl.ds(r0, chunk), :], kv[j, 0, :keys, :], (((1,), (1,)), ((), ())), preferred_element_type=f32
        )

    for m in range(2):
        for b in range(total // chunk):
            r0, keys = m * total + b * chunk, (b + 1) * chunk
            sc = scores_of(r0, z, keys)
            qpos = b * chunk + lax.broadcasted_iota(jnp.int32, (chunk, keys), 0)
            kpos = lax.broadcasted_iota(jnp.int32, (chunk, keys), 1)
            sc = jnp.where(kpos <= qpos, sc, -jnp.inf)
            top = jnp.max(sc, axis=1, keepdims=True)
            p = jnp.exp(sc - top)
            run_max[pl.ds(r0, chunk), :] = jnp.broadcast_to(top, (chunk, 128))
            run_sum[pl.ds(r0, chunk), :] = jnp.broadcast_to(jnp.sum(p, axis=1, keepdims=True), (chunk, 128))
            acc[pl.ds(r0, chunk), :] = jnp.dot(p.astype(bf16), kv[z, 1, :keys, :], preferred_element_type=f32)

    def block(d, carry):
        j = z - d
        @pl.when(d == 1)
        def _():
            await_chunk(0, s - 2)
            over(0, s - 2)
            next_above(0)

        kv_forward(j).wait_recv()

        @pl.when(has_up)
        def _():
            kv_forward(j).start()

            @pl.when(j == 0)
            def _():
                onward(0, s - 2, above)
                pl.when(z == 1)(down_up)

        @pl.when(d == 1)
        def _():
            next_above(1)
            next_above(2)

        def tile(b, inner):
            r0 = pl.multiple_of(b * chunk, chunk)
            here = pl.ds(r0, chunk)
            sc = scores_of(r0, j, total)
            old = run_max[here, :]
            top = jnp.maximum(old, jnp.max(sc, axis=1, keepdims=True))
            p = jnp.exp(sc - top[:, :1])
            shrink = jnp.exp(old - top)
            run_max[here, :] = top
            run_sum[here, :] = run_sum[here, :] * shrink + jnp.sum(p, axis=1, keepdims=True)
            acc[here, :] = acc[here, :] * shrink + jnp.dot(p.astype(bf16), kv[j, 1], preferred_element_type=f32)
            return inner

        lax.fori_loop(0, 2 * total // chunk, tile, 0)
        return carry

    lax.fori_loop(1, z + 1, block, 0)

    lam = lam_ref[y]
    differ = acc[:total, :] / run_sum[:total, :] - lam * (acc[total:, :] / run_sum[total:, :])
    spread = lax.rsqrt(jnp.mean(differ * differ, axis=1, keepdims=True) + 1e-06)
    att[...] = (differ * spread * gain_ref[...]).astype(bf16)

    head = 2 * t + y
    head_cols = pl.ds(pl.multiple_of(head * wide, wide), wide)

    def to_token(e, i, head_index):
        cols = pl.ds(pl.multiple_of(head_index * wide, wide), wide)
        return remote(
            att.at[pl.ds(e * rows + i * piece, piece)], ah_ref.at[:, cols],
            a_send.at[e * tp + i], a_recv.at[head_index], (2 * z + e, i),
        )

    mine = pltpu.make_async_copy(
        att.at[pl.ds(pl.multiple_of(y * rows + t * piece, piece), piece)], ah_ref.at[:, head_cols], loc.at[6]
    )
    mine.start()
    for e in range(2):
        for i in range(tp):
            pl.when(jnp.logical_or(e != y, i != t))(lambda: to_token(e, i, head).start())

    def up_below(d):
        @pl.when(z - d >= 0)
        def _():
            arrive(0, s - 2 * d, above, has_up)
            pl.when(jnp.logical_and(d == z, has_up))(down_up)

    @pl.when(z == 0)
    def _():
        for c in range(3):
            next_above(c)

    @pl.when(z + 1 < steps)
    def _():
        for c in range(3):
            over(c, s + 2)

    up_below(2)
    local[5].wait()
    mine.wait()
    for i in range(2 * tp):
        e, who = i % 2, i // 2
        pl.when(jnp.logical_or(e != y, who != t))(lambda: to_token(0, 0, i).wait_recv())

    projected = jnp.dot(ah_ref[...], ow[...], preferred_element_type=f32).astype(bf16)
    summed = (tok_ref[...].astype(f32) + projected.astype(f32)).astype(bf16)
    resid[...] = summed
    summed = summed.astype(f32)
    scale = lax.rsqrt(jnp.mean(summed * summed, axis=1, keepdims=True) + 1e-06)

    tc = t + 1 - 2 * lax.rem(t, 2)
    tx = lax.rem(t + 2, tp)
    td = lax.rem(tc + 2, tp)

    def band(i):
        return pl.ds(pl.multiple_of(i * piece, piece), piece)

    normed[band(t), :] = (summed * scale * mix_ref[...]).astype(bf16)

    def gathered(k, block_index, device):
        block_ref = normed.at[band(block_index)]
        return remote(block_ref, block_ref, ag_send.at[k], ag_recv.at[block_index], (s, device))

    gathered(0, t, tx).start()
    gathered(1, t, tc).start()

    def pump(d, carry):
        pl.when(d > 2)(lambda: up_below(d))
        from_above(d)
        return carry

    lax.fori_loop(2, min(3, steps), pump, 0)
    gathered(0, tx, tx).wait_recv()
    gathered(2, tx, tc).start()
    lax.fori_loop(min(3, steps), steps, pump, 0)
    gathered(1, tc, tc).wait_recv()
    gathered(2, td, tc).wait_recv()
    local[3].wait()
    local[4].wait()

    def order(k):
        return jnp.where(k < steps - z, z + k, steps - 1 - k)

    def across(c, i):
        j = 2 * i + 1 - y
        remote(shard(c, j), shard(c, j), y_send.at[j, c], w_recv.at[j, c], peer).wait_recv()

    def down_below(i):
        @pl.when(jnp.logical_and(i >= 0, i < z))
        def _():
            arrive(1, 2 * i + y, above, has_up)
            arrive(2, 2 * i + y, above, has_up)

    down_below(z - 1)
    pair_depth = 2 * up_ref.shape[0]
    hsum[...] = jnp.zeros_like(hsum)

    def up_pair(k, carry):
        i = order(k)
        across(0, i)
        span = pl.ds(pl.multiple_of(i * pair_depth, pair_depth), pair_depth)
        hsum[...] += jnp.dot(normed[:, span], upf_ref[span, :], preferred_element_type=f32)
        return carry

    lax.fori_loop(0, steps, up_pair, 0)
    hid[...] = jnp.square(jnp.maximum(hsum[...], 0.0)).astype(bf16)

    def to_core(j, m):
        return remote(
            part.at[j, band(tc if m == 0 else td)], core_in.at[j, m], c_send.at[j, m], c_recv.at[j, m], (s, tc)
        )

    def to_cross(j):
        return remote(cross.at[j], cross_in.at[j], x_send.at[j], x_recv.at[j], (s, tx))

    def add_cores(i):
        for e in range(2):
            j = 2 * i + e
            to_core(j, 1).wait_recv()
            cross[j] = (part[j, band(tx), :].astype(f32) + core_in[j, 1].astype(f32)).astype(bf16)
            to_cross(j).start()

    def down_pair(k, carry):
        i = order(k)
        later = order(k + 1)

        pl.when(jnp.logical_and(k + 1 < steps, later < z - 1))(lambda: down_below(later))
        pl.when(k > 0)(lambda: add_cores(order(k - 1)))
        across(1, i)
        across(2, i)
        for e in range(2):
            j = 2 * i + e
            part[j] = jnp.dot(hid[...], dnf_ref[j], preferred_element_type=f32).astype(bf16)
            to_core(j, 1).start()
            to_core(j, 0).start()
        return carry

    lax.fori_loop(0, steps, down_pair, 0)
    add_cores(order(steps - 1))

    cols = dn_ref.shape[1]
    for j in range(n):
        to_core(j, 0).wait_recv()
        to_cross(j).wait_recv()
        here = slice(j * cols, (j + 1) * cols)
        both = part[j, band(t), :].astype(f32) + core_in[j, 0].astype(f32) + cross_in[j].astype(f32)
        out_ref[:, here] = (resid[:, here].astype(f32) + both).astype(bf16)

    gathered(0, t, tx).wait_send()
    gathered(1, t, tc).wait_send()
    gathered(2, tx, tc).wait_send()
    for j in range(n):
        to_core(j, 0).wait_send()
        to_core(j, 1).wait_send()
        to_cross(j).wait_send()
    for copy in ex:
        copy.wait_send()
    for e in range(2):
        for i in range(tp):
            pl.when(jnp.logical_or(e != y, i != t))(lambda: to_token(e, i, head).wait_send())

    @pl.when(has_up)
    def _():
        def sent(j, carry):
            kv_forward(j).wait_send()
            return carry

        lax.fori_loop(0, z + 1, sent, 0)

    def line_sent(i, carry):
        j = 2 * i + y
        for c in range(3):
            moved = shard(c, j)
            remote(moved, moved, y_send.at[j, c], w_recv.at[j, c], peer).wait_send()
            gone = jnp.logical_or(jnp.logical_and(i <= z, has_up), jnp.logical_and(i > z, has_down))
            pl.when(gone)(lambda: remote(moved, moved, w_send.at[j, c], w_recv.at[j, c], peer).wait_send())
        return carry

    lax.fori_loop(0, steps, line_sent, 0)

    @pl.when(has_down)
    def _():
        for c in range(3):
            remote(own[c], shard(c, s), own_send.at[c], w_recv.at[s, c], below).wait_send()


def per_device(
    n, tp, tokens, queries, keys, values, lambdas, head_gain, out_weight, mixer_gain, up_weight, down_weight
):
    rows, wide = queries.shape[0], queries.shape[1] // 2
    depth, units = up_weight.shape
    cols = down_weight.shape[1]
    piece, width = tokens.shape
    vmem = pl.BlockSpec(memory_space=pltpu.VMEM)
    dma = pltpu.SemaphoreType.DMA
    return pl.pallas_call(
        functools.partial(layer_kernel, n, tp),
        out_shape=jax.ShapeDtypeStruct(tokens.shape, bf16),
        in_specs=[pl.BlockSpec(memory_space=pltpu.SMEM)] + [vmem] * 8 + [pl.BlockSpec(memory_space=pl.ANY)],
        out_specs=vmem,
        scratch_shapes=[
            pltpu.VMEM((piece, 2 * tp * wide), bf16),
            pltpu.VMEM((n * depth, units), bf16),
            pltpu.VMEM((n, units, cols), bf16),
            pltpu.VMEM((2 * rows, wide), bf16),
            pltpu.VMEM((n // 2, 2, 2 * rows, wide), bf16),
            pltpu.VMEM((4 * rows, wide), bf16),
            pltpu.VMEM((4 * rows, 128), f32),
            pltpu.VMEM((4 * rows, 128), f32),
            pltpu.VMEM((4 * rows, wide), f32),
            pltpu.VMEM((2 * rows, wide), bf16),
            pltpu.VMEM(out_weight.shape, bf16),
            pltpu.VMEM((piece, width), bf16),
            pltpu.VMEM((rows, width), bf16),
            pltpu.VMEM((rows, units), f32),
            pltpu.VMEM((rows, units), bf16),
            pltpu.VMEM((n, rows, cols), bf16),
            pltpu.VMEM((n, 2, piece, cols), bf16),
            pltpu.VMEM((n, piece, cols), bf16),
            pltpu.VMEM((n, piece, cols), bf16),
            dma((3,)), dma((3,)), dma((n // 2,)), dma((n // 2,)),
            dma((n, 3)), dma((3,)), dma((n, 3)), dma((n, 3)), dma((2 * tp,)), dma((2 * tp,)), dma((7,)),
            dma((3,)), dma((tp,)), dma((n, 2)), dma((n, 2)), dma((n,)), dma((n,)),
        ],
        compiler_params=pltpu.CompilerParams(
            collective_id=0, has_side_effects=True, vmem_limit_bytes=60 * 1024 * 1024
        ),
    )(
        lambdas, queries, keys, values, head_gain.reshape(1, -1), up_weight, down_weight,
        tokens, mixer_gain.reshape(1, -1), out_weight,
    )


def solution(mesh):
    placed = (
        P(("sp", "tp"), None),
        P("sp", "tp"),
        P("sp", "tp"),
        P("sp", "tp"),
        P("tp"),
        P(),
        P(),
        P(),
        P("sp", "tp"),
        P("tp", "sp"),
    )
    return jax.shard_map(
        functools.partial(per_device, mesh.shape["sp"], mesh.shape["tp"]),
        mesh=mesh,
        in_specs=placed,
        out_specs=P(("sp", "tp"), None),
        check_vma=False,
    )
```

```python
import functools

import jax
import jax.numpy as jnp
from jax import lax
from jax.experimental import pallas as pl
from jax.experimental.pallas import tpu as pltpu
from jax.sharding import PartitionSpec as P

DQK = 64
MESH = pl.DeviceIdType.MESH
f32, bf16 = jnp.float32, jnp.bfloat16


def layer_kernel(
    n, tp,
    lam_ref, q_ref, k_ref, v_ref, gain_ref, up_ref, dn_ref, tok_ref, mix_ref, ow_hbm,
    out_ref,
    ah_ref, upf_ref, dnf_ref,
    qb, kv, qm, run_max, run_sum, acc, att, ow, resid, normed, hsum, hid, part, core_in, cross, cross_in,
    ex_send, ex_recv, kv_send, kv_recv, w_send, own_send, y_send, w_recv, a_send, a_recv, loc,
    ag_send, ag_recv, c_send, c_recv, x_send, x_recv,
):
    s = lax.axis_index("sp")
    t = lax.axis_index("tp")
    z, y = s // 2, lax.rem(s, 2)
    steps = n // 2
    rows = q_ref.shape[0]
    wide = q_ref.shape[1] // 2
    peer = (s + 1 - 2 * y, t)
    above, below = (s + 2, t), (s - 2, t)
    has_up, has_down = z < steps - 1, z > 0
    piece = rows // tp

    barrier = pltpu.get_barrier_semaphore()

    def greet(device):
        pl.semaphore_signal(barrier, inc=1, device_id=device, device_id_type=MESH)

    for e in range(2):
        for i in range(tp):
            who = (2 * z + e, i)

            @pl.when(jnp.logical_or(e != y, i != t))
            def _():
                greet(who)

    pl.when(has_up)(lambda: greet(above))
    pl.when(has_down)(lambda: greet(below))
    pl.semaphore_wait(barrier, 2 * tp - 1 + has_up.astype(jnp.int32) + has_down.astype(jnp.int32))

    def remote(src, dst, send, recv, device):
        return pltpu.make_async_remote_copy(
            src_ref=src, dst_ref=dst, send_sem=send, recv_sem=recv, device_id=device, device_id_type=MESH
        )

    my_rows = pl.ds(pl.multiple_of(y * rows, rows), rows)
    peer_rows = pl.ds(pl.multiple_of((1 - y) * rows, rows), rows)
    my_cols = pl.ds(pl.multiple_of(y * wide, wide), wide)
    peer_cols = pl.ds(pl.multiple_of((1 - y) * wide, wide), wide)
    ex = []
    for i, (src, dst) in enumerate(((k_ref, kv.at[z, 0]), (v_ref, kv.at[z, 1]), (q_ref, qb))):
        ex.append(remote(src.at[:, peer_cols], dst.at[my_rows], ex_send.at[i], ex_recv.at[i], peer))
        ex[-1].start()

    half = dn_ref.shape[0] // 2
    halves = (slice(0, half), slice(half, 2 * half))

    def shard(c, j):
        if c == 0:
            depth = up_ref.shape[0]
            return upf_ref.at[pl.ds(pl.multiple_of(j * depth, depth), depth)]
        return dnf_ref.at[j, halves[c - 1]]

    own = (up_ref, dn_ref.at[halves[0]], dn_ref.at[halves[1]])

    def own_up(c):
        remote(own[c], shard(c, s), w_send.at[s, c], w_recv.at[s, c], above).start()

    pl.when(has_up)(lambda: own_up(0))
    for c in range(3):

        @pl.when(has_down)
        def _():
            remote(own[c], shard(c, s), own_send.at[c], w_recv.at[s, c], below).start()

        remote(own[c], shard(c, s), y_send.at[s, c], w_recv.at[s, c], peer).start()
    local = []
    for i, (src, dst) in enumerate(
        (
            (k_ref.at[:, my_cols], kv.at[z, 0, my_rows]),
            (v_ref.at[:, my_cols], kv.at[z, 1, my_rows]),
            (q_ref.at[:, my_cols], qb.at[my_rows]),
            (up_ref, shard(0, s)),
            (dn_ref, dnf_ref.at[s]),
            (ow_hbm, ow),
        )
    ):
        local.append(pltpu.make_async_copy(src, dst, loc.at[i]))
        local[-1].start()
    for i in range(3):
        local[i].wait()
    for i, (src, dst) in enumerate(((k_ref, kv.at[z, 0]), (v_ref, kv.at[z, 1]), (q_ref, qb))):
        remote(src.at[:, peer_cols], dst.at[peer_rows], ex_send.at[i], ex_recv.at[i], peer).wait_recv()

    def onward(c, j, device):
        moved = shard(c, j)
        remote(moved, moved, w_send.at[j, c], w_recv.at[j, c], device).start()

    def await_chunk(c, j):
        moved = shard(c, j)
        remote(moved, moved, w_send.at[j, c], w_recv.at[j, c], peer).wait_recv()

    def over(c, j):
        moved = shard(c, j)
        remote(moved, moved, y_send.at[j, c], w_recv.at[j, c], peer).start()

    def arrive(c, j, device, exists):
        await_chunk(c, j)
        over(c, j)
        pl.when(exists)(lambda: onward(c, j, device))

    def next_above(c):
        @pl.when(z + 1 < steps)
        def _():
            await_chunk(c, s + 2)
            pl.when(has_down)(lambda: onward(c, s + 2, below))

    def down_up():
        own_up(1)
        own_up(2)

    def from_above(d):
        for c in range(3):
            pl.when(z + d < steps)(lambda: arrive(c, s + 2 * d, below, has_down))

    def kv_forward(j):
        return remote(kv.at[j], kv.at[j], kv_send.at[j], kv_recv.at[j], above)

    @pl.when(has_up)
    def _():
        kv_forward(z).start()
        pl.when(jnp.logical_or(z == 0, z == steps - 2))(down_up)

    total = 2 * rows
    lane = lax.broadcasted_iota(jnp.int32, (total, wide), 1)
    scaled = qb[...] * jnp.asarray(DQK ** -0.5, bf16)
    for m in range(2):
        qm[m * total:(m + 1) * total, :] = jnp.where((lane < DQK) == (m == 0), scaled, jnp.zeros_like(scaled))

    chunk = min(256, total)

    def scores_of(r0, j, keys):
        return lax.dot_general(
            qm[pl.ds(r0, chunk), :], kv[j, 0, :keys, :], (((1,), (1,)), ((), ())), preferred_element_type=f32
        )

    for m in range(2):
        for b in range(total // chunk):
            r0, keys = m * total + b * chunk, (b + 1) * chunk
            sc = scores_of(r0, z, keys)
            qpos = b * chunk + lax.broadcasted_iota(jnp.int32, (chunk, keys), 0)
            kpos = lax.broadcasted_iota(jnp.int32, (chunk, keys), 1)
            sc = jnp.where(kpos <= qpos, sc, -jnp.inf)
            top = jnp.max(sc, axis=1, keepdims=True)
            p = jnp.exp(sc - top)
            run_max[pl.ds(r0, chunk), :] = jnp.broadcast_to(top, (chunk, 128))
            run_sum[pl.ds(r0, chunk), :] = jnp.broadcast_to(jnp.sum(p, axis=1, keepdims=True), (chunk, 128))
            acc[pl.ds(r0, chunk), :] = jnp.dot(p.astype(bf16), kv[z, 1, :keys, :], preferred_element_type=f32)

    def block(d, carry):
        j = z - d
        @pl.when(d == 1)
        def _():
            await_chunk(0, s - 2)
            over(0, s - 2)
            next_above(0)

        @pl.when(jnp.logical_and(d == 2, z == steps - 1))
        def _():
            for c in (1, 2):
                await_chunk(c, s - 2)
                over(c, s - 2)

        kv_forward(j).wait_recv()

        @pl.when(has_up)
        def _():
            kv_forward(j).start()

            @pl.when(j == 0)
            def _():
                onward(0, s - 2, above)
                if steps != 3:
                    pl.when(z == 1)(down_up)

        @pl.when(d == 1)
        def _():
            next_above(1)
            next_above(2)

        def tile(b, inner):
            r0 = pl.multiple_of(b * chunk, chunk)
            here = pl.ds(r0, chunk)
            sc = scores_of(r0, j, total)
            old = run_max[here, :]
            top = jnp.maximum(old, jnp.max(sc, axis=1, keepdims=True))
            p = jnp.exp(sc - top[:, :1])
            shrink = jnp.exp(old - top)
            run_max[here, :] = top
            run_sum[here, :] = run_sum[here, :] * shrink + jnp.sum(p, axis=1, keepdims=True)
            acc[here, :] = acc[here, :] * shrink + jnp.dot(p.astype(bf16), kv[j, 1], preferred_element_type=f32)
            return inner

        lax.fori_loop(0, 2 * total // chunk, tile, 0)
        return carry

    lax.fori_loop(1, z + 1, block, 0)

    lam = lam_ref[y]
    differ = acc[:total, :] / run_sum[:total, :] - lam * (acc[total:, :] / run_sum[total:, :])
    spread = lax.rsqrt(jnp.mean(differ * differ, axis=1, keepdims=True) + 1e-06)
    att[...] = (differ * spread * gain_ref[...]).astype(bf16)

    head = 2 * t + y
    head_cols = pl.ds(pl.multiple_of(head * wide, wide), wide)

    def to_token(e, i, head_index):
        cols = pl.ds(pl.multiple_of(head_index * wide, wide), wide)
        return remote(
            att.at[pl.ds(e * rows + i * piece, piece)], ah_ref.at[:, cols],
            a_send.at[e * tp + i], a_recv.at[head_index], (2 * z + e, i),
        )

    mine = pltpu.make_async_copy(
        att.at[pl.ds(pl.multiple_of(y * rows + t * piece, piece), piece)], ah_ref.at[:, head_cols], loc.at[6]
    )
    mine.start()
    for e in range(2):
        for i in range(tp):
            pl.when(jnp.logical_or(e != y, i != t))(lambda: to_token(e, i, head).start())

    def up_below(d):
        @pl.when(z - d >= 0)
        def _():
            arrive(0, s - 2 * d, above, has_up)
            pl.when(jnp.logical_and(d == z, z < steps - 2))(down_up)

    @pl.when(z == 0)
    def _():
        for c in range(3):
            next_above(c)

    @pl.when(z + 1 < steps)
    def _():
        for c in range(3):
            over(c, s + 2)

    up_below(2)
    local[5].wait()
    mine.wait()
    for i in range(2 * tp):
        e, who = i % 2, i // 2
        pl.when(jnp.logical_or(e != y, who != t))(lambda: to_token(0, 0, i).wait_recv())

    projected = jnp.dot(ah_ref[...], ow[...], preferred_element_type=f32).astype(bf16)
    summed = (tok_ref[...].astype(f32) + projected.astype(f32)).astype(bf16)
    resid[...] = summed
    summed = summed.astype(f32)
    scale = lax.rsqrt(jnp.mean(summed * summed, axis=1, keepdims=True) + 1e-06)

    tc = t + 1 - 2 * lax.rem(t, 2)
    tx = lax.rem(t + 2, tp)
    td = lax.rem(tc + 2, tp)

    def band(i):
        return pl.ds(pl.multiple_of(i * piece, piece), piece)

    normed[band(t), :] = (summed * scale * mix_ref[...]).astype(bf16)

    def gathered(k, block_index, device):
        block_ref = normed.at[band(block_index)]
        return remote(block_ref, block_ref, ag_send.at[k], ag_recv.at[block_index], (s, device))

    gathered(0, t, tx).start()
    gathered(1, t, tc).start()

    def pump(d, carry):
        pl.when(d > 2)(lambda: up_below(d))
        from_above(d)
        return carry

    lax.fori_loop(2, min(3, steps), pump, 0)
    gathered(0, tx, tx).wait_recv()
    gathered(2, tx, tc).start()
    lax.fori_loop(min(3, steps), steps, pump, 0)
    gathered(1, tc, tc).wait_recv()
    gathered(2, td, tc).wait_recv()
    local[3].wait()
    local[4].wait()

    def order(k):
        return jnp.where(k < steps - z, z + k, steps - 1 - k)

    def across(c, i):
        j = 2 * i + 1 - y
        remote(shard(c, j), shard(c, j), y_send.at[j, c], w_recv.at[j, c], peer).wait_recv()

    def down_below(i):
        @pl.when(jnp.logical_and(i >= 0, i < z))
        def _():
            arrive(1, 2 * i + y, above, has_up)
            arrive(2, 2 * i + y, above, has_up)

    pl.when(jnp.logical_or(z < steps - 1, z < 2))(lambda: down_below(z - 1))
    pair_depth = 2 * up_ref.shape[0]
    hsum[...] = jnp.zeros_like(hsum)

    def up_pair(k, carry):
        i = order(k)
        across(0, i)
        span = pl.ds(pl.multiple_of(i * pair_depth, pair_depth), pair_depth)
        hsum[...] += jnp.dot(normed[:, span], upf_ref[span, :], preferred_element_type=f32)
        return carry

    lax.fori_loop(0, steps, up_pair, 0)
    hid[...] = jnp.square(jnp.maximum(hsum[...], 0.0)).astype(bf16)

    def to_core(j, m):
        return remote(
            part.at[j, band(tc if m == 0 else td)], core_in.at[j, m], c_send.at[j, m], c_recv.at[j, m], (s, tc)
        )

    def to_cross(j):
        return remote(cross.at[j], cross_in.at[j], x_send.at[j], x_recv.at[j], (s, tx))

    def add_cores(i):
        for e in range(2):
            j = 2 * i + e
            to_core(j, 1).wait_recv()
            cross[j] = (part[j, band(tx), :].astype(f32) + core_in[j, 1].astype(f32)).astype(bf16)
            to_cross(j).start()

    def down_pair(k, carry):
        i = order(k)
        later = order(k + 1)

        pl.when(jnp.logical_and(k + 1 < steps, later < z - 1))(lambda: down_below(later))
        pl.when(k > 0)(lambda: add_cores(order(k - 1)))
        across(1, i)
        across(2, i)
        for e in range(2):
            j = 2 * i + e
            part[j] = jnp.dot(hid[...], dnf_ref[j], preferred_element_type=f32).astype(bf16)
            to_core(j, 1).start()
            to_core(j, 0).start()
        return carry

    lax.fori_loop(0, steps, down_pair, 0)
    add_cores(order(steps - 1))

    cols = dn_ref.shape[1]
    for j in range(n):
        to_core(j, 0).wait_recv()
        to_cross(j).wait_recv()
        here = slice(j * cols, (j + 1) * cols)
        both = part[j, band(t), :].astype(f32) + core_in[j, 0].astype(f32) + cross_in[j].astype(f32)
        out_ref[:, here] = (resid[:, here].astype(f32) + both).astype(bf16)

    gathered(0, t, tx).wait_send()
    gathered(1, t, tc).wait_send()
    gathered(2, tx, tc).wait_send()
    for j in range(n):
        to_core(j, 0).wait_send()
        to_core(j, 1).wait_send()
        to_cross(j).wait_send()
    for copy in ex:
        copy.wait_send()
    for e in range(2):
        for i in range(tp):
            pl.when(jnp.logical_or(e != y, i != t))(lambda: to_token(e, i, head).wait_send())

    @pl.when(has_up)
    def _():
        def sent(j, carry):
            kv_forward(j).wait_send()
            return carry

        lax.fori_loop(0, z + 1, sent, 0)

    def line_sent(i, carry):
        j = 2 * i + y
        for c in range(3):
            moved = shard(c, j)
            remote(moved, moved, y_send.at[j, c], w_recv.at[j, c], peer).wait_send()
            gone = jnp.logical_or(jnp.logical_and(i <= z, has_up), jnp.logical_and(i > z, has_down))
            pl.when(gone)(lambda: remote(moved, moved, w_send.at[j, c], w_recv.at[j, c], peer).wait_send())
        return carry

    lax.fori_loop(0, steps, line_sent, 0)

    @pl.when(has_down)
    def _():
        for c in range(3):
            remote(own[c], shard(c, s), own_send.at[c], w_recv.at[s, c], below).wait_send()


def per_device(
    n, tp, tokens, queries, keys, values, lambdas, head_gain, out_weight, mixer_gain, up_weight, down_weight
):
    rows, wide = queries.shape[0], queries.shape[1] // 2
    depth, units = up_weight.shape
    cols = down_weight.shape[1]
    piece, width = tokens.shape
    vmem = pl.BlockSpec(memory_space=pltpu.VMEM)
    dma = pltpu.SemaphoreType.DMA
    return pl.pallas_call(
        functools.partial(layer_kernel, n, tp),
        out_shape=jax.ShapeDtypeStruct(tokens.shape, bf16),
        in_specs=[pl.BlockSpec(memory_space=pltpu.SMEM)] + [vmem] * 8 + [pl.BlockSpec(memory_space=pl.ANY)],
        out_specs=vmem,
        scratch_shapes=[
            pltpu.VMEM((piece, 2 * tp * wide), bf16),
            pltpu.VMEM((n * depth, units), bf16),
            pltpu.VMEM((n, units, cols), bf16),
            pltpu.VMEM((2 * rows, wide), bf16),
            pltpu.VMEM((n // 2, 2, 2 * rows, wide), bf16),
            pltpu.VMEM((4 * rows, wide), bf16),
            pltpu.VMEM((4 * rows, 128), f32),
            pltpu.VMEM((4 * rows, 128), f32),
            pltpu.VMEM((4 * rows, wide), f32),
            pltpu.VMEM((2 * rows, wide), bf16),
            pltpu.VMEM(out_weight.shape, bf16),
            pltpu.VMEM((piece, width), bf16),
            pltpu.VMEM((rows, width), bf16),
            pltpu.VMEM((rows, units), f32),
            pltpu.VMEM((rows, units), bf16),
            pltpu.VMEM((n, rows, cols), bf16),
            pltpu.VMEM((n, 2, piece, cols), bf16),
            pltpu.VMEM((n, piece, cols), bf16),
            pltpu.VMEM((n, piece, cols), bf16),
            dma((3,)), dma((3,)), dma((n // 2,)), dma((n // 2,)),
            dma((n, 3)), dma((3,)), dma((n, 3)), dma((n, 3)), dma((2 * tp,)), dma((2 * tp,)), dma((7,)),
            dma((3,)), dma((tp,)), dma((n, 2)), dma((n, 2)), dma((n,)), dma((n,)),
        ],
        compiler_params=pltpu.CompilerParams(
            collective_id=0, has_side_effects=True, vmem_limit_bytes=60 * 1024 * 1024
        ),
    )(
        lambdas, queries, keys, values, head_gain.reshape(1, -1), up_weight, down_weight,
        tokens, mixer_gain.reshape(1, -1), out_weight,
    )


def solution(mesh):
    placed = (
        P(("sp", "tp"), None),
        P("sp", "tp"),
        P("sp", "tp"),
        P("sp", "tp"),
        P("tp"),
        P(),
        P(),
        P(),
        P("sp", "tp"),
        P("tp", "sp"),
    )
    return jax.shard_map(
        functools.partial(per_device, mesh.shape["sp"], mesh.shape["tp"]),
        mesh=mesh,
        in_specs=placed,
        out_specs=P(("sp", "tp"), None),
        check_vma=False,
    )
```
